32 devices in a mesh: tp: 8 (over z, core), dp: 4 (over y, x).
Axes of the slice: x: 2, y: 2, z: 4, core: 2. Of those that a mesh axis runs over, the one named last changes fastest.
Arguments:
- tokens: bfloat16 [32, 4096], P('tp', 'dp'), may hold values from -6 to 6
- norm_gain: bfloat16 [2, 4096], P(None, 'dp'), may hold values from 0.099609375 to 1.8984375
- w_query: bfloat16 [2, 4096, 1024], P(None, 'dp', 'tp'), may hold values from -0.09375 to 0.09375
- w_key: bfloat16 [2, 4096, 1024], P(None, 'dp', 'tp'), may hold values from -0.09375 to 0.09375
- w_value: bfloat16 [2, 4096, 1024], P(None, 'dp', 'tp'), may hold values from -0.09375 to 0.09375
- w_outgate: bfloat16 [2, 4096, 1024], P(None, 'dp', 'tp'), may hold values from -0.09375 to 0.09375
- w_gates: bfloat16 [2, 4096, 16], P(None, 'dp'), may hold values from -0.09375 to 0.09375
- gate_bias: float32 [2, 2, 8], P(None, None, 'tp'), may hold values from -1 to 5
- w_out: bfloat16 [2, 1024, 4096], P(None, 'tp', 'dp'), may hold values from -0.1875 to 0.1875
- memory: float32 [2, 32, 8, 128, 128], P(None, 'dp', 'tp'), may hold values from -6 to 6
- normalizer: float32 [2, 32, 8, 128], P(None, 'dp', 'tp'), may hold values from -3 to 3
- stabilizer: float32 [2, 32, 8], P(None, 'dp', 'tp'), may hold values from -8 to 300, as said below
Outputs:
- mixed: bfloat16 [32, 4096], P('tp', 'dp')
- new_memory: float32 [2, 32, 8, 128, 128], P(None, 'dp', 'tp')
- new_normalizer: float32 [2, 32, 8, 128], P(None, 'dp', 'tp')
- new_stabilizer: float32 [2, 32, 8], P(None, 'dp', 'tp')
The draws below stay inside these ranges and needn't reach their ends.
Inputs may be any that keep to these rules, and one draw needn't show every extreme that they name: `stabilizer`: lies between -8 and 8, except that some entries may be as large as 300.
All inputs are finite; a program needn't handle non-finite values.
Results may differ from the reference program's by a relative error of at most 0.04.
Values may be sent and summed in bfloat16 or wider, within the bound.
A program may use at most 64 MiB of HBM per device.

```python
import jax
import jax.numpy as jnp
from jax import lax

D = 4096
HEAD_SIZE = 128
HEADS = 8
SEQS = 32


def draw_stabilizer(key, part):
    shape = (2, SEQS, HEADS)
    values = jnp.clip(2.0 * jax.random.normal(jax.random.fold_in(key, 11), shape, jnp.float32), -8.0, 8.0)
    return values


def shard_levels(own_key, dims, shards, least, high):
    factor_of, own = 1.0, jax.random.fold_in(own_key, 6)
    for dim, shards_of in shards:
        draws = jnp.exp(jax.random.uniform(jax.random.fold_in(own, dim), (shards_of,), jnp.float32, least / len(shards), high / len(shards)))
        factor_of = factor_of * jnp.repeat(draws, dims[dim] // shards_of).reshape([-1 if axis == dim else 1 for axis in range(len(dims))])
    return factor_of


def scatter_about(key, dims, deviation, most, shards=(), held_as=jnp.bfloat16):
    drawn = jax.random.normal(key, dims, jnp.float32) * deviation
    if len(shards) > 0:
        drawn = shard_levels(key, dims, shards, -0.22, 0.18) * drawn
    return jnp.clip(drawn, min=-most, max=most).astype(held_as)


def setup_inputs(seed: int = 0) -> dict:
    splits = jax.random.split(jax.random.key(seed), 13)
    return {
        "tokens": scatter_about(splits[0], (SEQS, D), 1.0, 6.0, ((0, 8), (1, 4))),
        "norm_gain": jnp.clip(1.0 + 0.18 * jax.random.normal(splits[1], (2, D), jnp.float32), 0.099609375, 1.8984375).astype(jnp.bfloat16),
        "w_query": scatter_about(splits[2], (2, D, HEADS * HEAD_SIZE), D ** -0.5, 0.09375, ((1, 4), (2, 8))),
        "w_key": scatter_about(splits[3], (2, D, HEADS * HEAD_SIZE), D ** -0.5, 0.09375, ((1, 4), (2, 8))),
        "w_value": scatter_about(splits[4], (2, D, HEADS * HEAD_SIZE), D ** -0.5, 0.09375, ((1, 4), (2, 8))),
        "w_outgate": scatter_about(splits[5], (2, D, HEADS * HEAD_SIZE), D ** -0.5, 0.09375, ((1, 4), (2, 8))),
        "w_gates": scatter_about(splits[6], (2, D, 2 * HEADS), D ** -0.5, 0.09375, ((1, 4),)),
        "gate_bias": jnp.clip(-1.0 + 6.0 * jax.random.uniform(splits[7], (2, 2, HEADS), jnp.float32) ** shard_levels(splits[7], (2, 2, HEADS), ((2, 8),), -0.2, 0.2), -1.0, 5.0),
        "w_out": scatter_about(splits[8], (2, HEADS * HEAD_SIZE, D), (HEADS * HEAD_SIZE) ** -0.5, 0.1875, ((1, 8), (2, 4))),
        "memory": scatter_about(splits[9], (2, SEQS, HEADS, HEAD_SIZE, HEAD_SIZE), 1.0, 6.0, ((1, 4), (2, 8)), jnp.float32),
        "normalizer": scatter_about(splits[10], (2, SEQS, HEADS, HEAD_SIZE), 0.5, 3.0, ((1, 4), (2, 8)), jnp.float32),
        "stabilizer": draw_stabilizer(jax.random.fold_in(splits[12], 71), 0),
    }


epsilon = 1e-06

def cell_update(query, key_rows, value_rows, input_pre, forget_pre, memory, normalizer, stabilizer):
    batch_size = query.shape[0]
    head_count = input_pre.shape[1]
    query_float = query.astype(jnp.float32).reshape(batch_size, head_count, -1)
    key_float = key_rows.astype(jnp.float32).reshape(batch_size, head_count, -1) * query_float.shape[2] ** (-0.5)
    value_float = value_rows.astype(jnp.float32).reshape(batch_size, head_count, -1)
    carried = jax.nn.log_sigmoid(forget_pre) + stabilizer
    new_max = jnp.maximum(carried, input_pre)
    keep_factor = jnp.exp(carried - new_max)
    write_factor = jnp.exp(input_pre - new_max)
    new_memory = keep_factor[:, :, None, None] * memory + write_factor[:, :, None, None] * value_float[:, :, :, None] * key_float[:, :, None, :]
    new_normalizer = keep_factor[:, :, None] * normalizer + write_factor[:, :, None] * key_float
    numerator = lax.optimization_barrier(jnp.sum(new_memory * query_float[:, :, None, :], axis=3))
    denominator = lax.optimization_barrier(jnp.sum(new_normalizer * query_float, axis=2))
    floor_value = jnp.maximum(jnp.abs(denominator), jnp.exp(-new_max))
    readout = numerator / jnp.maximum(floor_value, 1.0)[:, :, None]
    return (readout.reshape(batch_size, -1), new_memory, new_normalizer, new_max)

def reference(tokens, norm_gain, w_query, w_key, w_value, w_outgate, w_gates, gate_bias, w_out, memory, normalizer, stabilizer):
    current = tokens
    memories = []
    normalizers = []
    maxima = []
    for layer_index in range(2):
        wide_rows = current.astype(jnp.float32)
        inv_scale = lax.rsqrt(lax.optimization_barrier(jnp.sum(wide_rows * wide_rows, axis=1)) / D + epsilon)[:, None]
        scaled = (wide_rows * norm_gain[layer_index].astype(jnp.float32)[None, :]).astype(jnp.bfloat16)
        query = (jnp.dot(scaled, w_query[layer_index], preferred_element_type=jnp.float32) * inv_scale).astype(jnp.bfloat16)
        key_rows = (jnp.dot(scaled, w_key[layer_index], preferred_element_type=jnp.float32) * inv_scale).astype(jnp.bfloat16)
        value_rows = (jnp.dot(scaled, w_value[layer_index], preferred_element_type=jnp.float32) * inv_scale).astype(jnp.bfloat16)
        outgate = (jnp.dot(scaled, w_outgate[layer_index], preferred_element_type=jnp.float32) * inv_scale).astype(jnp.bfloat16)
        gate_pre = jnp.dot(scaled, w_gates[layer_index], preferred_element_type=jnp.float32) * inv_scale
        input_pre = gate_pre[:, :HEADS] + gate_bias[layer_index, 0][None, :]
        forget_pre = gate_pre[:, HEADS:] + gate_bias[layer_index, 1][None, :]
        readout, new_memory, new_normalizer, new_max = cell_update(query, key_rows, value_rows, input_pre, forget_pre, memory[layer_index], normalizer[layer_index], stabilizer[layer_index])
        gated = (jax.nn.sigmoid(outgate.astype(jnp.float32)) * readout).astype(jnp.bfloat16)
        projected = jnp.dot(gated, w_out[layer_index], preferred_element_type=jnp.float32)
        current = (wide_rows + projected).astype(jnp.bfloat16)
        memories.append(new_memory)
        normalizers.append(new_normalizer)
        maxima.append(new_max)
    return (current, jnp.stack(memories), jnp.stack(normalizers), jnp.stack(maxima))
```

```python
import functools

import jax
import jax.numpy as jnp
from jax import lax
from jax.experimental import pallas as pl
from jax.experimental.pallas import tpu as pltpu
from jax.sharding import PartitionSpec as P

HEAD_SIZE = 128
MESH = pl.DeviceIdType.MESH
EPSILON = 1e-06
F32 = jnp.float32
BF16 = jnp.bfloat16


def kernel(
    n_tp,
    n_dp,
    tokens,
    norm_gain,
    w_query,
    w_key,
    w_value,
    w_outgate,
    w_gates,
    gate_bias,
    w_out,
    memory,
    normalizer,
    stabilizer,
    mixed,
    new_memory,
    new_normalizer,
    new_stabilizer,
    gain_v,
    w_in_v,
    w_gates_v,
    bias_v,
    w_out_v,
    mem_v,
    norm_v,
    stab_v,
    new_mem_v,
    own_x,
    x_slots,
    send_q,
    recv_q,
    send_g,
    recv_g,
    own_gated,
    gated_slots,
    send_o,
    recv_o,
    in_sem,
    w_sem,
    mem_sem,
    out_sem,
    ag_send,
    ag_recv,
    rq_send,
    rq_recv,
    rg_send,
    rg_recv,
    gd_send,
    gd_recv,
    ro_send,
    ro_recv,
):
    tp = lax.axis_index("tp")
    dp = lax.axis_index("dp")
    seqs = mem_v.shape[1]
    rows = own_x.shape[1]
    width = own_x.shape[2]
    total = n_tp * rows
    heads = w_gates_v.shape[1] // 2
    features = width * n_dp

    def tp_peer(off):
        return lax.rem(tp + off, n_tp)

    def dp_peer(off):
        return lax.rem(dp + off, n_dp)

    barrier = pltpu.get_barrier_semaphore()
    tok_copy = pltpu.make_async_copy(tokens, own_x.at[0], in_sem.at[0])
    tok_copy.start()
    for off in range(1, n_tp):
        pl.semaphore_signal(barrier, inc=1, device_id={"tp": tp_peer(off)}, device_id_type=MESH)
    for off in range(1, n_dp):
        pl.semaphore_signal(barrier, inc=1, device_id={"dp": dp_peer(off)}, device_id_type=MESH)

    small = [
        pltpu.make_async_copy(norm_gain, gain_v, in_sem.at[1]),
        pltpu.make_async_copy(w_gates, w_gates_v, in_sem.at[2]),
        pltpu.make_async_copy(gate_bias, bias_v, in_sem.at[3]),
        pltpu.make_async_copy(normalizer, norm_v, in_sem.at[4]),
        pltpu.make_async_copy(stabilizer, stab_v, in_sem.at[5]),
    ]
    for copy in small:
        copy.start()
    w_copies, out_copies, mem_copies = [], [], []
    for layer in range(2):
        w_copies.append(
            [
                pltpu.make_async_copy(
                    ref.at[layer],
                    w_in_v.at[layer, :, pl.ds(i * HEAD_SIZE, HEAD_SIZE)],
                    w_sem.at[layer, i],
                )
                for i, ref in enumerate((w_query, w_key, w_value, w_outgate))
            ]
        )
        mem_copies.append(pltpu.make_async_copy(memory.at[layer], mem_v.at[layer], mem_sem.at[layer]))
        out_copies.append(pltpu.make_async_copy(w_out.at[layer], w_out_v.at[layer], w_sem.at[layer, 4]))
        for copy in w_copies[layer]:
            copy.start()
        mem_copies[layer].start()
        out_copies[layer].start()

    tok_copy.wait()
    pl.semaphore_wait(barrier, n_tp + n_dp - 2)

    started = []

    def send_tp(src, dst, send_sem, recv_sem, off):
        copy = pltpu.make_async_remote_copy(
            src_ref=src,
            dst_ref=dst,
            send_sem=send_sem,
            recv_sem=recv_sem,
            device_id={"tp": tp_peer(off)},
            device_id_type=MESH,
        )
        copy.start()
        started.append(copy)
        return copy

    def send_dp(src, dst, send_sem, recv_sem, off):
        copy = pltpu.make_async_remote_copy(
            src_ref=src,
            dst_ref=dst,
            send_sem=send_sem,
            recv_sem=recv_sem,
            device_id={"dp": dp_peer(off)},
            device_id_type=MESH,
        )
        copy.start()
        started.append(copy)
        return copy

    def gather_x(layer):
        copies = [
            send_tp(
                own_x.at[layer],
                x_slots.at[layer, tp],
                ag_send.at[layer, off],
                ag_recv.at[layer, off],
                off,
            )
            for off in range(1, n_tp)
        ]
        x_slots[layer, tp] = own_x[layer]
        return copies

    lane = lax.broadcasted_iota(jnp.int32, (total, HEAD_SIZE), 1)
    diag_seq = lax.broadcasted_iota(jnp.int32, (seqs, seqs), 0) == lax.broadcasted_iota(
        jnp.int32, (seqs, seqs), 1
    )
    sub = lax.broadcasted_iota(jnp.int32, (seqs, HEAD_SIZE), 0)
    scale = HEAD_SIZE ** (-0.5)
    nt = (((1,), (1,)), ((), ()))
    tn = (((0,), (0,)), ((), ()))
    updates = []

    ag = gather_x(0)
    for copy in small:
        copy.wait()
    for layer in range(2):
        for copy in w_copies[layer]:
            copy.wait()
        mem_copies[layer].wait()
        mem = mem_v[layer].reshape(seqs * HEAD_SIZE, HEAD_SIZE)
        mem_hi = mem.astype(BF16)
        mem_lo = (mem - mem_hi.astype(F32)).astype(BF16)
        gain = gain_v[pl.ds(layer, 1), :].astype(F32)

        for copy in ag:
            copy.wait_recv()
        wide = jnp.concatenate([x_slots[layer, t].astype(F32) for t in range(n_tp)], axis=0)
        scaled = (wide * gain).astype(BF16)
        terms = jnp.dot(scaled, w_in_v[layer], preferred_element_type=F32).astype(BF16)
        for d in range(n_dp):
            send_q[layer, d] = terms[d * seqs : (d + 1) * seqs]
        rq = [
            send_dp(
                send_q.at[layer, dp_peer(off)],
                recv_q.at[layer, off],
                rq_send.at[layer, off],
                rq_recv.at[layer, off],
                off,
            )
            for off in range(1, n_dp)
        ]
        squares = jnp.sum(wide * wide, axis=1, keepdims=True)
        gates = lax.dot_general(scaled, w_gates_v[layer], nt, preferred_element_type=F32)
        column = lax.broadcasted_iota(jnp.int32, gates.shape, 1)
        gate_in = jnp.sum(jnp.where(column == tp, gates, 0.0), axis=1, keepdims=True)
        gate_forget = jnp.sum(jnp.where(column == heads + tp, gates, 0.0), axis=1, keepdims=True)
        packed = jnp.where(
            lane == 0, gate_in, jnp.where(lane == 1, gate_forget, jnp.where(lane == 2, squares, 0.0))
        )
        for d in range(n_dp):
            send_g[layer, d] = packed[d * seqs : (d + 1) * seqs]
        rg = [
            send_dp(
                send_g.at[layer, dp_peer(off)],
                recv_g.at[layer, off],
                rg_send.at[layer, off],
                rg_recv.at[layer, off],
                off,
            )
            for off in range(1, n_dp)
        ]

        sums = send_q[layer, dp].astype(F32)
        small_sums = send_g[layer, dp]
        for off in range(1, n_dp):
            rq[off - 1].wait_recv()
            sums = sums + recv_q[layer, off].astype(F32)
        for off in range(1, n_dp):
            rg[off - 1].wait_recv()
            small_sums = small_sums + recv_g[layer, off]
        inv = lax.rsqrt(small_sums[:, 2:3] / features + EPSILON)
        held = (sums * inv).astype(BF16)
        query = held[:, :HEAD_SIZE]
        key = held[:, HEAD_SIZE : 2 * HEAD_SIZE]
        value = held[:, 2 * HEAD_SIZE : 3 * HEAD_SIZE]
        outgate = held[:, 3 * HEAD_SIZE :].astype(F32)
        bias = bias_v[layer]
        pre_in = small_sums[:, 0:1] * inv + bias[:, 0:1]
        pre_forget = small_sums[:, 1:2] * inv + bias[:, 1:2]
        old_max = jnp.sum(
            jnp.where(diag_seq, jnp.broadcast_to(stab_v[layer], (seqs, seqs)), 0.0),
            axis=1,
            keepdims=True,
        )
        carried = jnp.minimum(pre_forget, 0.0) - jnp.log1p(jnp.exp(-jnp.abs(pre_forget))) + old_max
        new_max = jnp.maximum(carried, pre_in)
        keep = jnp.exp(carried - new_max)
        write = jnp.exp(pre_in - new_max)
        query_f = query.astype(F32)
        key_f = key.astype(F32) * scale
        value_f = value.astype(F32)
        new_norm = keep * norm_v[layer].reshape(seqs, HEAD_SIZE) + write * key_f
        denominator = jnp.sum(new_norm * query_f, axis=1, keepdims=True)
        key_query = jnp.sum(key_f * query_f, axis=1, keepdims=True)
        read = lax.dot_general(query, mem_hi, nt, preferred_element_type=F32) + lax.dot_general(
            query, mem_lo, nt, preferred_element_type=F32
        )
        old_read = jnp.zeros((seqs, HEAD_SIZE), F32)
        for s in range(seqs):
            old_read = old_read + jnp.where(
                sub == s, read[:, s * HEAD_SIZE : (s + 1) * HEAD_SIZE], 0.0
            )
        numerator = keep * old_read + (write * key_query) * value_f
        floor_value = jnp.maximum(jnp.maximum(jnp.abs(denominator), jnp.exp(-new_max)), 1.0)
        gated = (jax.nn.sigmoid(outgate) * (numerator / floor_value)).astype(BF16)
        own_gated[layer] = gated

        gd = [
            send_dp(
                own_gated.at[layer],
                gated_slots.at[layer, dp],
                gd_send.at[layer, off],
                gd_recv.at[layer, off],
                off,
            )
            for off in range(1, n_dp)
        ]
        gated_slots[layer, dp] = gated
        new_normalizer[layer] = new_norm.reshape(seqs, 1, HEAD_SIZE)
        new_stabilizer[layer] = jnp.sum(
            jnp.where(diag_seq, jnp.broadcast_to(new_max, (seqs, seqs)), 0.0), axis=0, keepdims=True
        )
        out_copies[layer].wait()
        for copy in gd:
            copy.wait_recv()
        all_gated = jnp.concatenate(
            [gated_slots[layer, d].astype(F32) for d in range(n_dp)], axis=0
        ).astype(BF16)
        partial = jnp.dot(all_gated, w_out_v[layer], preferred_element_type=F32)

        for t in range(n_tp):
            send_o[layer, t] = partial[t * rows : (t + 1) * rows].astype(BF16)
        ro = [
            send_tp(
                send_o.at[layer, tp_peer(off)],
                recv_o.at[layer, off],
                ro_send.at[layer, off],
                ro_recv.at[layer, off],
                off,
            )
            for off in range(1, n_tp)
        ]

        key_wide = jnp.concatenate(
            [jnp.where(sub == s, key.astype(F32), 0.0).astype(BF16) for s in range(seqs)], axis=1
        )
        outer = lax.dot_general(value, key_wide, tn, preferred_element_type=F32)
        write_scaled = write * scale
        for s in range(seqs):
            new_mem_v[layer, s, 0] = (
                keep[s : s + 1] * mem_v[layer, s, 0]
                + write_scaled[s : s + 1] * outer[:, s * HEAD_SIZE : (s + 1) * HEAD_SIZE]
            )
        update = pltpu.make_async_copy(new_mem_v.at[layer], new_memory.at[layer], out_sem.at[layer])
        update.start()
        updates.append(update)

        summed = send_o[layer, tp].astype(F32)
        for off in range(1, n_tp):
            ro[off - 1].wait_recv()
            summed = summed + recv_o[layer, off].astype(F32)
        result = (own_x[layer].astype(F32) + summed).astype(BF16)
        if layer == 0:
            own_x[1] = result
            ag = gather_x(1)
        else:
            mixed[...] = result
    for copy in started:
        copy.wait_send()
    for copy in updates:
        copy.wait()


def body(
    n_tp,
    n_dp,
    tokens,
    norm_gain,
    w_query,
    w_key,
    w_value,
    w_outgate,
    w_gates,
    gate_bias,
    w_out,
    memory,
    normalizer,
    stabilizer,
):
    rows, width = tokens.shape
    seqs, heads_here = memory.shape[1:3]
    assert heads_here == 1
    gate_columns = w_gates.shape[2]
    hbm = pl.BlockSpec(memory_space=pl.ANY)
    vmem = pl.BlockSpec(memory_space=pltpu.VMEM)
    dma = pltpu.SemaphoreType.DMA
    moved = 2 * (5 * width * HEAD_SIZE * 2 + 2 * seqs * HEAD_SIZE * HEAD_SIZE * 4)
    mixed, new_memory, new_normalizer, new_stabilizer = pl.pallas_call(
        functools.partial(kernel, n_tp, n_dp),
        out_shape=(
            jax.ShapeDtypeStruct(tokens.shape, BF16),
            jax.ShapeDtypeStruct(memory.shape, F32),
            jax.ShapeDtypeStruct(normalizer.shape, F32),
            jax.ShapeDtypeStruct((2, heads_here, seqs), F32),
        ),
        in_specs=[hbm] * 12,
        out_specs=(vmem, hbm, vmem, vmem),
        scratch_shapes=[
            pltpu.VMEM((2, width), BF16),
            pltpu.VMEM((2, width, 4 * HEAD_SIZE), BF16),
            pltpu.VMEM((2, gate_columns, width), BF16),
            pltpu.VMEM((2, 1, 2), F32),
            pltpu.VMEM((2, HEAD_SIZE, width), BF16),
            pltpu.VMEM(memory.shape, F32),
            pltpu.VMEM(normalizer.shape, F32),
            pltpu.VMEM((2, 1, seqs), F32),
            pltpu.VMEM(memory.shape, F32),
            pltpu.VMEM((2, rows, width), BF16),
            pltpu.VMEM((2, n_tp, rows, width), BF16),
            pltpu.VMEM((2, n_dp, seqs, 4 * HEAD_SIZE), BF16),
            pltpu.VMEM((2, n_dp, seqs, 4 * HEAD_SIZE), BF16),
            pltpu.VMEM((2, n_dp, seqs, HEAD_SIZE), F32),
            pltpu.VMEM((2, n_dp, seqs, HEAD_SIZE), F32),
            pltpu.VMEM((2, seqs, HEAD_SIZE), BF16),
            pltpu.VMEM((2, n_dp, seqs, HEAD_SIZE), BF16),
            pltpu.VMEM((2, n_tp, rows, width), BF16),
            pltpu.VMEM((2, n_tp, rows, width), BF16),
            dma((6,)),
            dma((2, 5)),
            dma((2,)),
            dma((2,)),
            dma((2, n_tp)),
            dma((2, n_tp)),
            dma((2, n_dp)),
            dma((2, n_dp)),
            dma((2, n_dp)),
            dma((2, n_dp)),
            dma((2, n_dp)),
            dma((2, n_dp)),
            dma((2, n_tp)),
            dma((2, n_tp)),
        ],
        compiler_params=pltpu.CompilerParams(
            collective_id=0, has_side_effects=True, vmem_limit_bytes=60 * 1024 * 1024
        ),
        cost_estimate=pl.CostEstimate(
            flops=2 * 2 * n_tp * rows * width * 5 * HEAD_SIZE, bytes_accessed=moved, transcendentals=0
        ),
    )(
        tokens,
        norm_gain,
        w_query,
        w_key,
        w_value,
        w_outgate,
        jnp.swapaxes(w_gates, 1, 2),
        jnp.swapaxes(gate_bias, 1, 2),
        w_out,
        memory,
        normalizer,
        jnp.swapaxes(stabilizer, 1, 2),
    )
    return mixed, new_memory, new_normalizer, jnp.swapaxes(new_stabilizer, 1, 2)


def solution(mesh):
    placed = (
        P("tp", "dp"),
        P(None, "dp"),
        P(None, "dp", "tp"),
        P(None, "dp", "tp"),
        P(None, "dp", "tp"),
        P(None, "dp", "tp"),
        P(None, "dp", None),
        P(None, None, "tp"),
        P(None, "tp", "dp"),
        P(None, "dp", "tp", None, None),
        P(None, "dp", "tp", None),
        P(None, "dp", "tp"),
    )
    return jax.shard_map(
        functools.partial(body, mesh.shape["tp"], mesh.shape["dp"]),
        mesh=mesh,
        in_specs=placed,
        out_specs=(
            P("tp", "dp"),
            P(None, "dp", "tp", None, None),
            P(None, "dp", "tp", None),
            P(None, "dp", "tp"),
        ),
        check_vma=False,
    )
```

```python
import functools

import jax
import jax.numpy as jnp
from jax import lax
from jax.experimental import pallas as pl
from jax.experimental.pallas import tpu as pltpu
from jax.sharding import PartitionSpec as P

HEAD_SIZE = 128
MESH = pl.DeviceIdType.MESH
EPSILON = 1e-06
F32 = jnp.float32
BF16 = jnp.bfloat16


def kernel(
    n_tp,
    n_dp,
    tokens,
    norm_gain,
    w_query,
    w_key,
    w_value,
    w_outgate,
    w_gates,
    gate_bias,
    w_out,
    memory,
    normalizer,
    stabilizer,
    mixed,
    new_memory,
    new_normalizer,
    new_stabilizer,
    gain_v,
    w_in_v,
    w_gates_v,
    bias_v,
    w_out_v,
    mem_v,
    norm_v,
    stab_v,
    own_x,
    x_slots,
    send_q,
    recv_q,
    send_g,
    recv_g,
    own_gated,
    gated_slots,
    send_o,
    recv_o,
    in_sem,
    w_sem,
    mem_sem,
    ag_send,
    ag_recv,
    rq_send,
    rq_recv,
    rg_send,
    rg_recv,
    gd_send,
    gd_recv,
    ro_send,
    ro_recv,
):
    tp = lax.axis_index("tp")
    dp = lax.axis_index("dp")
    seqs = mem_v.shape[1]
    rows = own_x.shape[1]
    width = own_x.shape[2]
    total = n_tp * rows
    heads = w_gates_v.shape[1] // 2
    features = width * n_dp

    def flip(index, mask):
        for bit in range(mask.bit_length()):
            if mask >> bit & 1:
                index = index + (1 - 2 * (index // 2**bit % 2)) * 2**bit
        return index

    def tp_peer(mask):
        return flip(tp, mask)

    def dp_peer(mask):
        return flip(dp, mask)

    tp_masks = range(n_tp - 1, 0, -1)
    dp_masks = range(n_dp - 1, 0, -1)

    barrier = pltpu.get_barrier_semaphore()
    tok_copy = pltpu.make_async_copy(tokens, own_x.at[0], in_sem.at[0])
    tok_copy.start()
    for off in tp_masks:
        pl.semaphore_signal(barrier, inc=1, device_id={"tp": tp_peer(off)}, device_id_type=MESH)
    for off in dp_masks:
        pl.semaphore_signal(barrier, inc=1, device_id={"dp": dp_peer(off)}, device_id_type=MESH)

    small = [
        pltpu.make_async_copy(norm_gain, gain_v, in_sem.at[1]),
        pltpu.make_async_copy(w_gates, w_gates_v, in_sem.at[2]),
        pltpu.make_async_copy(gate_bias, bias_v, in_sem.at[3]),
        pltpu.make_async_copy(normalizer, norm_v, in_sem.at[4]),
        pltpu.make_async_copy(stabilizer, stab_v, in_sem.at[5]),
    ]
    for copy in small:
        copy.start()
    w_copies, out_copies, mem_copies = [], [], []
    for layer in range(2):
        w_copies.append(
            [
                pltpu.make_async_copy(
                    ref.at[layer],
                    w_in_v.at[layer, :, pl.ds(i * HEAD_SIZE, HEAD_SIZE)],
                    w_sem.at[layer, i],
                )
                for i, ref in enumerate((w_query, w_key, w_value, w_outgate))
            ]
        )
        mem_copies.append(pltpu.make_async_copy(memory.at[layer], mem_v.at[layer], mem_sem.at[layer]))
        out_copies.append(pltpu.make_async_copy(w_out.at[layer], w_out_v.at[layer], w_sem.at[layer, 4]))
        for copy in w_copies[layer]:
            copy.start()
        mem_copies[layer].start()
        out_copies[layer].start()

    tok_copy.wait()
    pl.semaphore_wait(barrier, n_tp + n_dp - 2)

    started = []

    def send_tp(src, dst, send_sem, recv_sem, off):
        copy = pltpu.make_async_remote_copy(
            src_ref=src,
            dst_ref=dst,
            send_sem=send_sem,
            recv_sem=recv_sem,
            device_id={"tp": tp_peer(off)},
            device_id_type=MESH,
        )
        copy.start()
        started.append(copy)
        return copy

    def send_dp(src, dst, send_sem, recv_sem, off):
        copy = pltpu.make_async_remote_copy(
            src_ref=src,
            dst_ref=dst,
            send_sem=send_sem,
            recv_sem=recv_sem,
            device_id={"dp": dp_peer(off)},
            device_id_type=MESH,
        )
        copy.start()
        started.append(copy)
        return copy

    def gather_x(layer):
        copies = [
            send_tp(
                own_x.at[layer],
                x_slots.at[layer, tp],
                ag_send.at[layer, off],
                ag_recv.at[layer, off],
                off,
            )
            for off in tp_masks
        ]
        x_slots[layer, tp] = own_x[layer]
        return copies

    lane = lax.broadcasted_iota(jnp.int32, (total, HEAD_SIZE), 1)
    diag_seq = lax.broadcasted_iota(jnp.int32, (seqs, seqs), 0) == lax.broadcasted_iota(
        jnp.int32, (seqs, seqs), 1
    )
    sub = lax.broadcasted_iota(jnp.int32, (seqs, HEAD_SIZE), 0)
    scale = HEAD_SIZE ** (-0.5)
    nt = (((1,), (1,)), ((), ()))
    tn = (((0,), (0,)), ((), ()))

    ag = gather_x(0)
    for copy in small:
        copy.wait()
    for layer in range(2):
        columns = w_gates_v[layer].astype(F32).T.astype(BF16)
        w_in_v[layer, :, 4 * HEAD_SIZE : 4 * HEAD_SIZE + 2 * heads] = columns
    for layer in range(2):
        for copy in w_copies[layer]:
            copy.wait()
        mem_copies[layer].wait()
        mem = mem_v[layer].reshape(seqs * HEAD_SIZE, HEAD_SIZE)
        mem_hi = mem.astype(BF16)
        mem_lo = (mem - mem_hi.astype(F32)).astype(BF16)
        gain = gain_v[pl.ds(layer, 1), :].astype(F32)

        for copy in ag:
            copy.wait_recv()
        wide = jnp.concatenate([x_slots[layer, t].astype(F32) for t in range(n_tp)], axis=0)
        scaled = (wide * gain).astype(BF16)
        terms = jnp.dot(scaled, w_in_v[layer], preferred_element_type=F32)
        squares = jnp.sum(wide * wide, axis=1, keepdims=True)
        gates = terms[:, 4 * HEAD_SIZE :]
        gate_in = jnp.sum(jnp.where(lane == tp, gates, 0.0), axis=1, keepdims=True)
        gate_forget = jnp.sum(jnp.where(lane == heads + tp, gates, 0.0), axis=1, keepdims=True)
        packed = jnp.where(
            lane == 0, gate_in, jnp.where(lane == 1, gate_forget, jnp.where(lane == 2, squares, 0.0))
        )
        for d in range(n_dp):
            send_q[layer, d] = terms[d * seqs : (d + 1) * seqs, : 4 * HEAD_SIZE].astype(BF16)
            send_g[layer, d] = packed[d * seqs : (d + 1) * seqs]
        rq, rg = [], []
        for off in dp_masks:
            rg.append(
                send_dp(
                    send_g.at[layer, dp_peer(off)],
                    recv_g.at[layer, off],
                    rg_send.at[layer, off],
                    rg_recv.at[layer, off],
                    off,
                )
            )
            rq.append(
                send_dp(
                    send_q.at[layer, dp_peer(off)],
                    recv_q.at[layer, off],
                    rq_send.at[layer, off],
                    rq_recv.at[layer, off],
                    off,
                )
            )

        sums = send_q[layer, dp].astype(F32)
        small_sums = send_g[layer, dp]
        for off in dp_masks:
            rq[n_dp - 1 - off].wait_recv()
            sums = sums + recv_q[layer, off].astype(F32)
        for off in dp_masks:
            rg[n_dp - 1 - off].wait_recv()
            small_sums = small_sums + recv_g[layer, off]
        inv = lax.rsqrt(small_sums[:, 2:3] / features + EPSILON)
        held = (sums * inv).astype(BF16)
        query = held[:, :HEAD_SIZE]
        key = held[:, HEAD_SIZE : 2 * HEAD_SIZE]
        value = held[:, 2 * HEAD_SIZE : 3 * HEAD_SIZE]
        outgate = held[:, 3 * HEAD_SIZE :].astype(F32)
        bias = bias_v[layer]
        pre_in = small_sums[:, 0:1] * inv + bias[:, 0:1]
        pre_forget = small_sums[:, 1:2] * inv + bias[:, 1:2]
        old_max = jnp.sum(
            jnp.where(diag_seq, jnp.broadcast_to(stab_v[layer], (seqs, seqs)), 0.0),
            axis=1,
            keepdims=True,
        )
        carried = jnp.minimum(pre_forget, 0.0) - jnp.log1p(jnp.exp(-jnp.abs(pre_forget))) + old_max
        new_max = jnp.maximum(carried, pre_in)
        keep = jnp.exp(carried - new_max)
        write = jnp.exp(pre_in - new_max)
        query_f = query.astype(F32)
        key_f = key.astype(F32) * scale
        value_f = value.astype(F32)
        new_norm = keep * norm_v[layer].reshape(seqs, HEAD_SIZE) + write * key_f
        denominator = jnp.sum(new_norm * query_f, axis=1, keepdims=True)
        key_query = jnp.sum(key_f * query_f, axis=1, keepdims=True)
        read = lax.dot_general(query, mem_hi, nt, preferred_element_type=F32) + lax.dot_general(
            query, mem_lo, nt, preferred_element_type=F32
        )
        old_read = jnp.zeros((seqs, HEAD_SIZE), F32)
        for s in range(seqs):
            old_read = old_read + jnp.where(
                sub == s, read[:, s * HEAD_SIZE : (s + 1) * HEAD_SIZE], 0.0
            )
        numerator = keep * old_read + (write * key_query) * value_f
        floor_value = jnp.maximum(jnp.maximum(jnp.abs(denominator), jnp.exp(-new_max)), 1.0)
        gated = (jax.nn.sigmoid(outgate) * (numerator / floor_value)).astype(BF16)
        own_gated[layer] = gated

        gd = [
            send_dp(
                own_gated.at[layer],
                gated_slots.at[layer, dp],
                gd_send.at[layer, off],
                gd_recv.at[layer, off],
                off,
            )
            for off in dp_masks
        ]
        gated_slots[layer, dp] = gated
        new_normalizer[layer] = new_norm.reshape(seqs, 1, HEAD_SIZE)
        new_stabilizer[layer] = jnp.sum(
            jnp.where(diag_seq, jnp.broadcast_to(new_max, (seqs, seqs)), 0.0), axis=0, keepdims=True
        )
        out_copies[layer].wait()
        for copy in gd:
            copy.wait_recv()
        all_gated = jnp.concatenate(
            [gated_slots[layer, d].astype(F32) for d in range(n_dp)], axis=0
        ).astype(BF16)
        partial = jnp.dot(all_gated, w_out_v[layer], preferred_element_type=F32)

        for t in range(n_tp):
            send_o[layer, t] = partial[t * rows : (t + 1) * rows].astype(BF16)
        ro = [
            send_tp(
                send_o.at[layer, tp_peer(off)],
                recv_o.at[layer, off],
                ro_send.at[layer, off],
                ro_recv.at[layer, off],
                off,
            )
            for off in tp_masks
        ]

        key_wide = jnp.concatenate(
            [jnp.where(sub == s, key.astype(F32), 0.0).astype(BF16) for s in range(seqs)], axis=1
        )
        outer = lax.dot_general(value, key_wide, tn, preferred_element_type=F32)
        write_scaled = write * scale
        for s in range(seqs):
            new_memory[layer, s, 0] = (
                keep[s : s + 1] * mem_v[layer, s, 0]
                + write_scaled[s : s + 1] * outer[:, s * HEAD_SIZE : (s + 1) * HEAD_SIZE]
            )

        summed = send_o[layer, tp].astype(F32)
        for off in tp_masks:
            ro[n_tp - 1 - off].wait_recv()
            summed = summed + recv_o[layer, off].astype(F32)
        result = (own_x[layer].astype(F32) + summed).astype(BF16)
        if layer == 0:
            own_x[1] = result
            ag = gather_x(1)
        else:
            mixed[...] = result
    for copy in started:
        copy.wait_send()


def write_out(*refs):
    sources, targets, sem = refs[:4], refs[4:8], refs[8]
    copies = [
        pltpu.make_async_copy(source, target, sem.at[i])
        for i, (source, target) in enumerate(zip(sources, targets))
    ]
    for copy in copies:
        copy.start()
    for copy in copies:
        copy.wait()


def body(
    n_tp,
    n_dp,
    tokens,
    norm_gain,
    w_query,
    w_key,
    w_value,
    w_outgate,
    w_gates,
    gate_bias,
    w_out,
    memory,
    normalizer,
    stabilizer,
):
    rows, width = tokens.shape
    seqs, heads_here = memory.shape[1:3]
    assert heads_here == 1
    gate_columns = w_gates.shape[2]
    hbm = pl.BlockSpec(memory_space=pl.ANY)
    vmem = pl.BlockSpec(memory_space=pltpu.VMEM)
    dma = pltpu.SemaphoreType.DMA
    moved = 2 * (5 * width * HEAD_SIZE * 2 + 2 * seqs * HEAD_SIZE * HEAD_SIZE * 4)
    results = pl.pallas_call(
        functools.partial(kernel, n_tp, n_dp),
        out_shape=(
            pltpu.VMEM(tokens.shape, BF16),
            pltpu.VMEM(memory.shape, F32),
            pltpu.VMEM(normalizer.shape, F32),
            pltpu.VMEM((2, heads_here, seqs), F32),
        ),
        in_specs=[hbm] * 12,
        out_specs=(vmem,) * 4,
        scratch_shapes=[
            pltpu.VMEM((2, width), BF16),
            pltpu.VMEM((2, width, 5 * HEAD_SIZE), BF16),
            pltpu.VMEM((2, gate_columns, width), BF16),
            pltpu.VMEM((2, 1, 2), F32),
            pltpu.VMEM((2, HEAD_SIZE, width), BF16),
            pltpu.VMEM(memory.shape, F32),
            pltpu.VMEM(normalizer.shape, F32),
            pltpu.VMEM((2, 1, seqs), F32),
            pltpu.VMEM((2, rows, width), BF16),
            pltpu.VMEM((2, n_tp, rows, width), BF16),
            pltpu.VMEM((2, n_dp, seqs, 4 * HEAD_SIZE), BF16),
            pltpu.VMEM((2, n_dp, seqs, 4 * HEAD_SIZE), BF16),
            pltpu.VMEM((2, n_dp, seqs, HEAD_SIZE), F32),
            pltpu.VMEM((2, n_dp, seqs, HEAD_SIZE), F32),
            pltpu.VMEM((2, seqs, HEAD_SIZE), BF16),
            pltpu.VMEM((2, n_dp, seqs, HEAD_SIZE), BF16),
            pltpu.VMEM((2, n_tp, rows, width), BF16),
            pltpu.VMEM((2, n_tp, rows, width), BF16),
            dma((6,)),
            dma((2, 5)),
            dma((2,)),
            dma((2, n_tp)),
            dma((2, n_tp)),
            dma((2, n_dp)),
            dma((2, n_dp)),
            dma((2, n_dp)),
            dma((2, n_dp)),
            dma((2, n_dp)),
            dma((2, n_dp)),
            dma((2, n_tp)),
            dma((2, n_tp)),
        ],
        compiler_params=pltpu.CompilerParams(
            collective_id=0, has_side_effects=True, vmem_limit_bytes=60 * 1024 * 1024
        ),
        cost_estimate=pl.CostEstimate(
            flops=2 * 2 * n_tp * rows * width * 5 * HEAD_SIZE, bytes_accessed=moved, transcendentals=0
        ),
    )(
        tokens,
        norm_gain,
        w_query,
        w_key,
        w_value,
        w_outgate,
        jnp.swapaxes(w_gates, 1, 2),
        jnp.swapaxes(gate_bias, 1, 2),
        w_out,
        memory,
        normalizer,
        jnp.swapaxes(stabilizer, 1, 2),
    )
    mixed, new_memory, new_normalizer, new_stabilizer = pl.pallas_call(
        write_out,
        out_shape=[jax.ShapeDtypeStruct(r.shape, r.dtype) for r in results],
        in_specs=[vmem] * 4,
        out_specs=[hbm] * 4,
        scratch_shapes=[dma((4,))],
    )(*(pltpu.with_memory_space_constraint(r, pltpu.VMEM) for r in results))
    return mixed, new_memory, new_normalizer, jnp.swapaxes(new_stabilizer, 1, 2)


def solution(mesh):
    placed = (
        P("tp", "dp"),
        P(None, "dp"),
        P(None, "dp", "tp"),
        P(None, "dp", "tp"),
        P(None, "dp", "tp"),
        P(None, "dp", "tp"),
        P(None, "dp", None),
        P(None, None, "tp"),
        P(None, "tp", "dp"),
        P(None, "dp", "tp", None, None),
        P(None, "dp", "tp", None),
        P(None, "dp", "tp"),
    )
    return jax.shard_map(
        functools.partial(body, mesh.shape["tp"], mesh.shape["dp"]),
        mesh=mesh,
        in_specs=placed,
        out_specs=(
            P("tp", "dp"),
            P(None, "dp", "tp", None, None),
            P(None, "dp", "tp", None),
            P(None, "dp", "tp"),
        ),
        check_vma=False,
    )
```

```python
import functools

import jax
import jax.numpy as jnp
from jax import lax
from jax.experimental import pallas as pl
from jax.experimental.pallas import tpu as pltpu
from jax.sharding import PartitionSpec as P

HEAD_SIZE = 128
MESH = pl.DeviceIdType.MESH
EPSILON = 1e-06
F32 = jnp.float32
BF16 = jnp.bfloat16


def kernel(
    n_tp,
    n_dp,
    tokens,
    norm_gain,
    w_query,
    w_key,
    w_value,
    w_outgate,
    w_gates,
    gate_bias,
    w_out,
    memory,
    normalizer,
    stabilizer,
    mixed,
    new_memory,
    new_normalizer,
    new_stabilizer,
    gain_v,
    w_in_v,
    w_gates_v,
    bias_v,
    w_out_v,
    mem_v,
    norm_v,
    stab_v,
    own_x,
    x_slots,
    send_q,
    recv_q,
    send_g,
    recv_g,
    own_gated,
    gated_slots,
    send_o,
    recv_o,
    send_p,
    recv_p,
    own_pair,
    recv_z,
    own_half,
    halves,
    in_sem,
    w_sem,
    mem_sem,
    ag_send,
    ag_recv,
    rq_send,
    rq_recv,
    rg_send,
    rg_recv,
    gd_send,
    gd_recv,
    ro_send,
    ro_recv,
    pair_send,
    pair_recv,
    z_send,
    z_recv,
):
    tp = lax.axis_index("tp")
    dp = lax.axis_index("dp")
    seqs = mem_v.shape[1]
    rows = own_x.shape[1]
    width = own_x.shape[2]
    total = n_tp * rows
    heads = w_gates_v.shape[1] // 2
    features = width * n_dp

    def flip(index, mask):
        for bit in range(mask.bit_length()):
            if mask >> bit & 1:
                index = index + (1 - 2 * (index // 2**bit % 2)) * 2**bit
        return index

    def tp_peer(mask):
        return flip(tp, mask)

    def dp_peer(mask):
        return flip(dp, mask)

    core = lax.rem(tp, 2)
    half = width // 2
    chip_masks = range(n_tp - 2, 0, -2)
    tp_masks = range(n_tp - 1, 0, -1)
    dp_masks = range(n_dp - 1, 0, -1)

    barrier = pltpu.get_barrier_semaphore()
    tok_copy = pltpu.make_async_copy(tokens, own_x.at[0], in_sem.at[0])
    tok_copy.start()
    for off in tp_masks:
        pl.semaphore_signal(barrier, inc=1, device_id={"tp": tp_peer(off)}, device_id_type=MESH)
    for off in dp_masks:
        pl.semaphore_signal(barrier, inc=1, device_id={"dp": dp_peer(off)}, device_id_type=MESH)

    small = [
        pltpu.make_async_copy(norm_gain, gain_v, in_sem.at[1]),
        pltpu.make_async_copy(w_gates, w_gates_v, in_sem.at[2]),
        pltpu.make_async_copy(gate_bias, bias_v, in_sem.at[3]),
        pltpu.make_async_copy(normalizer, norm_v, in_sem.at[4]),
        pltpu.make_async_copy(stabilizer, stab_v, in_sem.at[5]),
    ]
    for copy in small:
        copy.start()
    w_copies, out_copies, mem_copies = [], [], []
    for layer in range(2):
        w_copies.append(
            [
                pltpu.make_async_copy(
                    ref.at[layer],
                    w_in_v.at[layer, :, pl.ds(i * HEAD_SIZE, HEAD_SIZE)],
                    w_sem.at[layer, i],
                )
                for i, ref in enumerate((w_query, w_key, w_value, w_outgate))
            ]
        )
        mem_copies.append(pltpu.make_async_copy(memory.at[layer], mem_v.at[layer], mem_sem.at[layer]))
        out_copies.append(pltpu.make_async_copy(w_out.at[layer], w_out_v.at[layer], w_sem.at[layer, 4]))
        for copy in w_copies[layer]:
            copy.start()
        mem_copies[layer].start()
        out_copies[layer].start()

    tok_copy.wait()
    pl.semaphore_wait(barrier, n_tp + n_dp - 2)

    started = []

    def send_tp(src, dst, send_sem, recv_sem, off):
        copy = pltpu.make_async_remote_copy(
            src_ref=src,
            dst_ref=dst,
            send_sem=send_sem,
            recv_sem=recv_sem,
            device_id={"tp": tp_peer(off)},
            device_id_type=MESH,
        )
        copy.start()
        started.append(copy)
        return copy

    def send_dp(src, dst, send_sem, recv_sem, off):
        copy = pltpu.make_async_remote_copy(
            src_ref=src,
            dst_ref=dst,
            send_sem=send_sem,
            recv_sem=recv_sem,
            device_id={"dp": dp_peer(off)},
            device_id_type=MESH,
        )
        copy.start()
        started.append(copy)
        return copy

    def gather_x(layer):
        copies = [
            send_tp(
                own_x.at[layer],
                x_slots.at[layer, tp],
                ag_send.at[layer, off],
                ag_recv.at[layer, off],
                off,
            )
            for off in tp_masks
        ]
        x_slots[layer, tp] = own_x[layer]
        return copies

    lane = lax.broadcasted_iota(jnp.int32, (total, HEAD_SIZE), 1)
    diag_seq = lax.broadcasted_iota(jnp.int32, (seqs, seqs), 0) == lax.broadcasted_iota(
        jnp.int32, (seqs, seqs), 1
    )
    sub = lax.broadcasted_iota(jnp.int32, (seqs, HEAD_SIZE), 0)
    scale = HEAD_SIZE ** (-0.5)
    nt = (((1,), (1,)), ((), ()))
    tn = (((0,), (0,)), ((), ()))

    ag = gather_x(0)
    for copy in small:
        copy.wait()
    for layer in range(2):
        columns = w_gates_v[layer].astype(F32).T.astype(BF16)
        w_in_v[layer, :, 4 * HEAD_SIZE : 4 * HEAD_SIZE + 2 * heads] = columns
    for layer in range(2):
        for copy in w_copies[layer]:
            copy.wait()
        mem_copies[layer].wait()
        mem = mem_v[layer].reshape(seqs * HEAD_SIZE, HEAD_SIZE)
        mem_hi = mem.astype(BF16)
        mem_lo = (mem - mem_hi.astype(F32)).astype(BF16)
        gain = gain_v[pl.ds(layer, 1), :].astype(F32)

        for copy in ag:
            copy.wait_recv()
        if layer == 0:
            wide = jnp.concatenate([x_slots[0, t].astype(F32) for t in range(n_tp)], axis=0)
        else:
            wide = jnp.concatenate([halves[0], halves[1]], axis=1).astype(F32)
        scaled = (wide * gain).astype(BF16)
        terms = jnp.dot(scaled, w_in_v[layer], preferred_element_type=F32)
        squares = jnp.sum(wide * wide, axis=1, keepdims=True)
        gates = terms[:, 4 * HEAD_SIZE :]
        gate_in = jnp.sum(jnp.where(lane == tp, gates, 0.0), axis=1, keepdims=True)
        gate_forget = jnp.sum(jnp.where(lane == heads + tp, gates, 0.0), axis=1, keepdims=True)
        packed = jnp.where(
            lane == 0, gate_in, jnp.where(lane == 1, gate_forget, jnp.where(lane == 2, squares, 0.0))
        )
        for d in range(n_dp):
            send_q[layer, d] = terms[d * seqs : (d + 1) * seqs, : 4 * HEAD_SIZE].astype(BF16)
            send_g[layer, d] = packed[d * seqs : (d + 1) * seqs]
        rq, rg = [], []
        for off in dp_masks:
            rg.append(
                send_dp(
                    send_g.at[layer, dp_peer(off)],
                    recv_g.at[layer, off],
                    rg_send.at[layer, off],
                    rg_recv.at[layer, off],
                    off,
                )
            )
            rq.append(
                send_dp(
                    send_q.at[layer, dp_peer(off)],
                    recv_q.at[layer, off],
                    rq_send.at[layer, off],
                    rq_recv.at[layer, off],
                    off,
                )
            )

        sums = send_q[layer, dp].astype(F32)
        small_sums = send_g[layer, dp]
        for off in dp_masks:
            rq[n_dp - 1 - off].wait_recv()
            sums = sums + recv_q[layer, off].astype(F32)
        for off in dp_masks:
            rg[n_dp - 1 - off].wait_recv()
            small_sums = small_sums + recv_g[layer, off]
        inv = lax.rsqrt(small_sums[:, 2:3] / features + EPSILON)
        held = (sums * inv).astype(BF16)
        query = held[:, :HEAD_SIZE]
        key = held[:, HEAD_SIZE : 2 * HEAD_SIZE]
        value = held[:, 2 * HEAD_SIZE : 3 * HEAD_SIZE]
        outgate = held[:, 3 * HEAD_SIZE :].astype(F32)
        bias = bias_v[layer]
        pre_in = small_sums[:, 0:1] * inv + bias[:, 0:1]
        pre_forget = small_sums[:, 1:2] * inv + bias[:, 1:2]
        old_max = jnp.sum(
            jnp.where(diag_seq, jnp.broadcast_to(stab_v[layer], (seqs, seqs)), 0.0),
            axis=1,
            keepdims=True,
        )
        carried = jnp.minimum(pre_forget, 0.0) - jnp.log1p(jnp.exp(-jnp.abs(pre_forget))) + old_max
        new_max = jnp.maximum(carried, pre_in)
        keep = jnp.exp(carried - new_max)
        write = jnp.exp(pre_in - new_max)
        query_f = query.astype(F32)
        key_f = key.astype(F32) * scale
        value_f = value.astype(F32)
        new_norm = keep * norm_v[layer].reshape(seqs, HEAD_SIZE) + write * key_f
        denominator = jnp.sum(new_norm * query_f, axis=1, keepdims=True)
        key_query = jnp.sum(key_f * query_f, axis=1, keepdims=True)
        read = lax.dot_general(query, mem_hi, nt, preferred_element_type=F32) + lax.dot_general(
            query, mem_lo, nt, preferred_element_type=F32
        )
        old_read = jnp.zeros((seqs, HEAD_SIZE), F32)
        for s in range(seqs):
            old_read = old_read + jnp.where(
                sub == s, read[:, s * HEAD_SIZE : (s + 1) * HEAD_SIZE], 0.0
            )
        numerator = keep * old_read + (write * key_query) * value_f
        floor_value = jnp.maximum(jnp.maximum(jnp.abs(denominator), jnp.exp(-new_max)), 1.0)
        gated = (jax.nn.sigmoid(outgate) * (numerator / floor_value)).astype(BF16)
        own_gated[layer] = gated

        gd = [
            send_dp(
                own_gated.at[layer],
                gated_slots.at[layer, dp],
                gd_send.at[layer, off],
                gd_recv.at[layer, off],
                off,
            )
            for off in dp_masks
        ]
        gated_slots[layer, dp] = gated
        new_normalizer[layer] = new_norm.reshape(seqs, 1, HEAD_SIZE)
        new_stabilizer[layer] = jnp.sum(
            jnp.where(diag_seq, jnp.broadcast_to(new_max, (seqs, seqs)), 0.0), axis=0, keepdims=True
        )
        out_copies[layer].wait()
        for copy in gd:
            copy.wait_recv()
        all_gated = jnp.concatenate(
            [gated_slots[layer, d].astype(F32) for d in range(n_dp)], axis=0
        ).astype(BF16)
        partial = jnp.dot(all_gated, w_out_v[layer], preferred_element_type=F32)

        def update_states():
            key_wide = jnp.concatenate(
                [jnp.where(sub == s, key.astype(F32), 0.0).astype(BF16) for s in range(seqs)], axis=1
            )
            outer = lax.dot_general(value, key_wide, tn, preferred_element_type=F32)
            write_scaled = write * scale
            for s in range(seqs):
                new_memory[layer, s, 0] = (
                    keep[s : s + 1] * mem_v[layer, s, 0]
                    + write_scaled[s : s + 1] * outer[:, s * HEAD_SIZE : (s + 1) * HEAD_SIZE]
                )

        if layer == 0:
            first, second = partial[:, :half], partial[:, half:]
            send_p[0] = first.astype(BF16)
            send_p[1] = second.astype(BF16)
            swap = send_tp(send_p.at[1 - core], recv_p, pair_send.at[0], pair_recv.at[0], 1)
            own_part = jnp.where(core == 0, first, second)
            swap.wait_recv()
            pair = (own_part + recv_p[...].astype(F32)).astype(BF16)
            own_pair[...] = pair
            copies = [
                send_tp(
                    own_pair, recv_z.at[mask // 2], z_send.at[mask // 2], z_recv.at[mask // 2], mask
                )
                for mask in chip_masks
            ]
            update_states()
            summed = jnp.where(core == 0, wide[:, :half], wide[:, half:]) + pair.astype(F32)
            for mask, copy in zip(chip_masks, copies):
                copy.wait_recv()
                summed = summed + recv_z[mask // 2].astype(F32)
            result = summed.astype(BF16)
            own_half[...] = result
            ag = [send_tp(own_half, halves.at[core], pair_send.at[1], pair_recv.at[1], 1)]
            halves[core] = result
        else:
            for t in range(n_tp):
                send_o[layer, t] = partial[t * rows : (t + 1) * rows].astype(BF16)
            ro = [
                send_tp(
                    send_o.at[layer, tp_peer(off)],
                    recv_o.at[layer, off],
                    ro_send.at[layer, off],
                    ro_recv.at[layer, off],
                    off,
                )
                for off in tp_masks
            ]
            update_states()
            summed = send_o[layer, tp].astype(F32)
            for t in range(n_tp):
                summed = summed + jnp.where(tp == t, wide[t * rows : (t + 1) * rows], 0.0)
            for copy, off in zip(ro, tp_masks):
                copy.wait_recv()
                summed = summed + recv_o[layer, off].astype(F32)
            mixed[...] = summed.astype(BF16)
    for copy in started:
        copy.wait_send()


def write_out(*refs):
    sources, targets, sem = refs[:4], refs[4:8], refs[8]
    copies = [
        pltpu.make_async_copy(source, target, sem.at[i])
        for i, (source, target) in enumerate(zip(sources, targets))
    ]
    for copy in copies:
        copy.start()
    for copy in copies:
        copy.wait()


def body(
    n_tp,
    n_dp,
    tokens,
    norm_gain,
    w_query,
    w_key,
    w_value,
    w_outgate,
    w_gates,
    gate_bias,
    w_out,
    memory,
    normalizer,
    stabilizer,
):
    rows, width = tokens.shape
    seqs, heads_here = memory.shape[1:3]
    assert heads_here == 1
    gate_columns = w_gates.shape[2]
    hbm = pl.BlockSpec(memory_space=pl.ANY)
    vmem = pl.BlockSpec(memory_space=pltpu.VMEM)
    dma = pltpu.SemaphoreType.DMA
    moved = 2 * (5 * width * HEAD_SIZE * 2 + 2 * seqs * HEAD_SIZE * HEAD_SIZE * 4)
    results = pl.pallas_call(
        functools.partial(kernel, n_tp, n_dp),
        out_shape=(
            pltpu.VMEM(tokens.shape, BF16),
            pltpu.VMEM(memory.shape, F32),
            pltpu.VMEM(normalizer.shape, F32),
            pltpu.VMEM((2, heads_here, seqs), F32),
        ),
        in_specs=[hbm] * 12,
        out_specs=(vmem,) * 4,
        scratch_shapes=[
            pltpu.VMEM((2, width), BF16),
            pltpu.VMEM((2, width, 5 * HEAD_SIZE), BF16),
            pltpu.VMEM((2, gate_columns, width), BF16),
            pltpu.VMEM((2, 1, 2), F32),
            pltpu.VMEM((2, HEAD_SIZE, width), BF16),
            pltpu.VMEM(memory.shape, F32),
            pltpu.VMEM(normalizer.shape, F32),
            pltpu.VMEM((2, 1, seqs), F32),
            pltpu.VMEM((2, rows, width), BF16),
            pltpu.VMEM((2, n_tp, rows, width), BF16),
            pltpu.VMEM((2, n_dp, seqs, 4 * HEAD_SIZE), BF16),
            pltpu.VMEM((2, n_dp, seqs, 4 * HEAD_SIZE), BF16),
            pltpu.VMEM((2, n_dp, seqs, HEAD_SIZE), F32),
            pltpu.VMEM((2, n_dp, seqs, HEAD_SIZE), F32),
            pltpu.VMEM((2, seqs, HEAD_SIZE), BF16),
            pltpu.VMEM((2, n_dp, seqs, HEAD_SIZE), BF16),
            pltpu.VMEM((2, n_tp, rows, width), BF16),
            pltpu.VMEM((2, n_tp, rows, width), BF16),
            pltpu.VMEM((2, n_tp * rows, width // 2), BF16),
            pltpu.VMEM((n_tp * rows, width // 2), BF16),
            pltpu.VMEM((n_tp * rows, width // 2), BF16),
            pltpu.VMEM((n_tp // 2, n_tp * rows, width // 2), BF16),
            pltpu.VMEM((n_tp * rows, width // 2), BF16),
            pltpu.VMEM((2, n_tp * rows, width // 2), BF16),
            dma((6,)),
            dma((2, 5)),
            dma((2,)),
            dma((2, n_tp)),
            dma((2, n_tp)),
            dma((2, n_dp)),
            dma((2, n_dp)),
            dma((2, n_dp)),
            dma((2, n_dp)),
            dma((2, n_dp)),
            dma((2, n_dp)),
            dma((2, n_tp)),
            dma((2, n_tp)),
            dma((2,)),
            dma((2,)),
            dma((n_tp // 2,)),
            dma((n_tp // 2,)),
        ],
        compiler_params=pltpu.CompilerParams(
            collective_id=0, has_side_effects=True, vmem_limit_bytes=60 * 1024 * 1024
        ),
        cost_estimate=pl.CostEstimate(
            flops=2 * 2 * n_tp * rows * width * 5 * HEAD_SIZE, bytes_accessed=moved, transcendentals=0
        ),
    )(
        tokens,
        norm_gain,
        w_query,
        w_key,
        w_value,
        w_outgate,
        jnp.swapaxes(w_gates, 1, 2),
        jnp.swapaxes(gate_bias, 1, 2),
        w_out,
        memory,
        normalizer,
        jnp.swapaxes(stabilizer, 1, 2),
    )
    mixed, new_memory, new_normalizer, new_stabilizer = pl.pallas_call(
        write_out,
        out_shape=[jax.ShapeDtypeStruct(r.shape, r.dtype) for r in results],
        in_specs=[vmem] * 4,
        out_specs=[hbm] * 4,
        scratch_shapes=[dma((4,))],
    )(*(pltpu.with_memory_space_constraint(r, pltpu.VMEM) for r in results))
    return mixed, new_memory, new_normalizer, jnp.swapaxes(new_stabilizer, 1, 2)


def solution(mesh):
    placed = (
        P("tp", "dp"),
        P(None, "dp"),
        P(None, "dp", "tp"),
        P(None, "dp", "tp"),
        P(None, "dp", "tp"),
        P(None, "dp", "tp"),
        P(None, "dp", None),
        P(None, None, "tp"),
        P(None, "tp", "dp"),
        P(None, "dp", "tp", None, None),
        P(None, "dp", "tp", None),
        P(None, "dp", "tp"),
    )
    return jax.shard_map(
        functools.partial(body, mesh.shape["tp"], mesh.shape["dp"]),
        mesh=mesh,
        in_specs=placed,
        out_specs=(
            P("tp", "dp"),
            P(None, "dp", "tp", None, None),
            P(None, "dp", "tp", None),
            P(None, "dp", "tp"),
        ),
        check_vma=False,
    )
```
